32 devices in a mesh: dp: 4 (over y, x), kv: 4 (over z), tp: 2 (over core).
Axes of the slice: x: 2, y: 2, z: 4, core: 2. Of those that a mesh axis runs over, the one named last changes fastest.
Arguments:
- tokens: bfloat16 [32, 4096], P('dp', 'kv'), may hold values from -6 to 6
- token_gain: float32 [4096], P('kv'), may hold values from 0.1 to 1.9
- asker_narrow_matrix: bfloat16 [4096, 1536], P('kv'), may hold values from -0.09375 to 0.09375
- hidden_narrow_matrix: bfloat16 [4096, 1088], P('kv'), may hold values from -0.09375 to 0.09375
- asker_multiplier: float32 [1536], replicated, may hold values from 0.1 to 1.9
- hidden_multiplier: float32 [1024], replicated, may hold values from 0.1 to 1.9
- asker_unspun_matrix: bfloat16 [1536, 64, 128], P(None, ('kv', 'tp')), may hold values from -0.15625 to 0.15625
- asker_spin_matrix: bfloat16 [1536, 64, 64], P(None, ('kv', 'tp')), may hold values from -0.15625 to 0.15625
- lock_widen_matrix: bfloat16 [64, 128, 1024], P(('kv', 'tp')), may hold values from -0.25 to 0.25
- payload_widen_matrix: bfloat16 [64, 1024, 128], P(('kv', 'tp')), may hold values from -0.75 to 0.75
- w_output: bfloat16 [8192, 4096], P(('kv', 'tp')), may hold values from -0.75 to 0.75
- cache_latent: bfloat16 [32, 1024, 1024], P('dp', 'kv'), may hold values from -4 to 4
- cache_rotary: bfloat16 [32, 1024, 64], P('dp', 'kv'), may hold values from -400 to 400
- lengths: int32 [32], P('dp'), may hold values from 512 to 1023, as said below
Outputs:
- attention_out: float32 [32, 4096], P('dp', ('kv', 'tp'))
- incoming_hidden: float32 [32, 1024], P('dp')
- incoming_spun: float32 [32, 64], P('dp')
The draws below stay inside these ranges and needn't reach their ends.
Inputs may be any that keep to these rules, and one draw needn't show every extreme that they name: `lengths`: each length lies in 512 to 1023; some sequence has 1023 and some has 512.
All inputs are finite; a program needn't handle non-finite values.
Results may differ from the reference program's by a relative error of at most 0.015.
Values may be sent and summed in bfloat16 or wider, within the bound.
A program may use at most 64 MiB of HBM per device.

```python
import jax
import jax.numpy as jnp
from jax import lax

MODEL_BREADTH = 4096
ASKER_COUNT = 64
ASK_PACKED = 1536
PACKED_BREADTH = 1024
PLAIN_SPAN = 128
SPIN_SPAN = 64
PAYLOAD_SPAN = 128
BATCH_COUNT = 32
MEMORY_SLOTS = 1024


def draw_cache_latent(key, part):
    shape = (BATCH_COUNT, MEMORY_SLOTS, PACKED_BREADTH)
    values = jnp.clip(jax.random.normal(key, shape, jnp.float32), -4.0, 4.0)
    return values.astype(jnp.bfloat16)


def draw_cache_rotary(key, part):
    shape = (BATCH_COUNT, MEMORY_SLOTS, SPIN_SPAN)
    values = jnp.clip(jax.random.normal(key, shape, jnp.float32), -4.0, 4.0)
    mighty = jax.random.uniform(jax.random.fold_in(key, 7), (BATCH_COUNT, 1, SPIN_SPAN), jnp.float32, -400.0, 400.0)
    chosen_rows = (jnp.arange(BATCH_COUNT) % 4 == 0)[:, None, None]
    slots = jnp.arange(MEMORY_SLOTS)[None, :, None]
    values = jnp.where(chosen_rows & (slots == 3), mighty, values)
    values = jnp.where(chosen_rows & (slots == 5), -mighty, values)
    return values.astype(jnp.bfloat16)


def draw_lengths(key, part):
    values = jax.random.randint(key, (BATCH_COUNT,), MEMORY_SLOTS // 2, MEMORY_SLOTS, dtype=jnp.int32)
    values = values.at[0].set(MEMORY_SLOTS - 1)
    return values.at[BATCH_COUNT - 1].set(MEMORY_SLOTS // 2)


def with_spikes(entries, rng, source, target, parts, factor):
    def block_of(axis_at):
        return (jnp.arange(entries.shape[axis_at]) // (entries.shape[axis_at] // parts)).reshape((-1,) + (1,) * (entries.ndim - 1 - axis_at))

    one_side = jax.random.permutation(rng, parts)[block_of(target)]
    far = (block_of(target) + parts // 2) % parts
    return jnp.where((block_of(source) == one_side) | (block_of(source) == far), factor * entries, entries)


def levels(rng, shape, cuts, smallest, high):
    def one(dim, parts):
        steps = jax.random.uniform(jax.random.fold_in(jax.random.fold_in(rng, 6), dim), (parts,), jnp.float32, smallest / len(cuts), high / len(cuts))
        return jnp.repeat(jnp.exp(steps), shape[dim] // parts).reshape((-1,) + (1,) * (len(shape) - dim - 1))

    level = one(*cuts[0])
    for cut in cuts[1:]:
        level = level * one(*cut)
    return level


def bell_draw(rng, dims, spread, limit, split=(), held_as=jnp.bfloat16):
    drawn = jax.random.normal(rng, dims, jnp.float32) * spread
    if len(split) > 0:
        drawn = levels(rng, dims, split, -0.22, 0.18) * drawn
    return jnp.clip(drawn, min=-limit, max=limit).astype(held_as)


def bell_draw_with(rng, extent, scale, reach, pieces, heavy, held_as=jnp.bfloat16):
    values = scale * jax.random.normal(rng, extent, jnp.float32)
    if pieces:
        values = values * levels(rng, extent, pieces, -0.22, 0.18)
    return jnp.clip(with_spikes(values, jax.random.fold_in(rng, 3), *heavy), -reach, reach).astype(held_as)


def setup_inputs(seed: int = 0) -> dict:
    streams_of = jax.random.split(jax.random.key(seed), 15)
    tokens = bell_draw(streams_of[0], (BATCH_COUNT, MODEL_BREADTH), 1.0, 6.0, ((0, 4), (1, 4)))
    token_gain = jnp.clip(1.0 + 0.18 * jax.random.normal(streams_of[1], (MODEL_BREADTH,), jnp.float32), 0.1, 1.9)
    asker_narrow_matrix = bell_draw(streams_of[2], (MODEL_BREADTH, ASK_PACKED), MODEL_BREADTH ** -0.5, 0.09375, ((0, 4),))
    hidden_narrow_matrix = bell_draw(streams_of[3], (MODEL_BREADTH, PACKED_BREADTH + SPIN_SPAN), MODEL_BREADTH ** -0.5, 0.09375, ((0, 4),))
    asker_multiplier = jnp.clip(1.0 + 0.18 * jax.random.normal(streams_of[4], (ASK_PACKED,), jnp.float32), 0.1, 1.9)
    hidden_multiplier = jnp.clip(1.0 + 0.18 * jax.random.normal(streams_of[5], (PACKED_BREADTH,), jnp.float32), 0.1, 1.9)
    asker_unspun_matrix = bell_draw(streams_of[6], (ASK_PACKED, ASKER_COUNT, PLAIN_SPAN), ASK_PACKED ** -0.5, 0.15625, ((1, 8),))
    asker_spin_matrix = bell_draw(streams_of[7], (ASK_PACKED, ASKER_COUNT, SPIN_SPAN), ASK_PACKED ** -0.5, 0.15625, ((1, 8),))
    lock_widen_matrix = bell_draw(streams_of[8], (ASKER_COUNT, PLAIN_SPAN, PACKED_BREADTH), (4 * PLAIN_SPAN) ** -0.5, 0.25, ((0, 8),))
    payload_widen_matrix = bell_draw(streams_of[9], (ASKER_COUNT, PACKED_BREADTH, PAYLOAD_SPAN), (PACKED_BREADTH // 16) ** -0.5, 0.75, ((0, 8),))
    w_output = bell_draw_with(streams_of[10], (ASKER_COUNT * PAYLOAD_SPAN, MODEL_BREADTH), (ASKER_COUNT * PAYLOAD_SPAN // 64) ** -0.5, 0.75, ((0, 8),), (0, 1, 8, 2.0))
    cache_latent = draw_cache_latent(jax.random.fold_in(streams_of[14], 71), 0)
    cache_rotary = draw_cache_rotary(jax.random.fold_in(streams_of[14], 71), 0)
    lengths = draw_lengths(jax.random.fold_in(streams_of[14], 71), 0)
    return dict(tokens=tokens, token_gain=token_gain, asker_narrow_matrix=asker_narrow_matrix, hidden_narrow_matrix=hidden_narrow_matrix, asker_multiplier=asker_multiplier, hidden_multiplier=hidden_multiplier, asker_unspun_matrix=asker_unspun_matrix, asker_spin_matrix=asker_spin_matrix, lock_widen_matrix=lock_widen_matrix, payload_widen_matrix=payload_widen_matrix, w_output=w_output, cache_latent=cache_latent, cache_rotary=cache_rotary, lengths=lengths)


EPS = 1e-06
THETA = 10000.0

def magnitude_divisor(values, gain):
    mean_square = lax.optimization_barrier(jnp.mean(values * values, axis=-1, keepdims=True))
    return values * lax.rsqrt(mean_square + EPS) * gain

def spinning(values, position):
    half_width = values.shape[-1] // 2
    exponent = jnp.arange(half_width, dtype=jnp.float32) * (2.0 / values.shape[-1])
    frequency = THETA ** (-exponent)
    angles = position.astype(jnp.float32)[:, None] * frequency[None, :]
    angles = angles.reshape((angles.shape[0],) + (1,) * (values.ndim - 2) + (half_width,))
    cosine = jnp.cos(angles)
    sine_table = jnp.sin(angles)
    former = values[..., :half_width]
    latter = values[..., half_width:]
    return jnp.concatenate([former * cosine - latter * sine_table, former * sine_table + latter * cosine], axis=-1)

def reference(tokens, token_gain, asker_narrow_matrix, hidden_narrow_matrix, asker_multiplier, hidden_multiplier, asker_unspun_matrix, asker_spin_matrix, lock_widen_matrix, payload_widen_matrix, w_output, cache_latent, cache_rotary, lengths):
    tokens_wide = tokens.astype(jnp.float32)
    squares = lax.optimization_barrier(jnp.sum(tokens_wide * tokens_wide, axis=1, keepdims=True))
    row_scale = lax.rsqrt(squares / MODEL_BREADTH + EPS)
    scaled = (tokens_wide * token_gain).astype(jnp.bfloat16)
    query_down = jnp.dot(scaled, asker_narrow_matrix, preferred_element_type=jnp.float32) * row_scale
    hidden_squeeze = jnp.dot(scaled, hidden_narrow_matrix, preferred_element_type=jnp.float32) * row_scale
    squeezed = magnitude_divisor(query_down, asker_multiplier).astype(jnp.bfloat16)
    incoming_hidden = magnitude_divisor(hidden_squeeze[:, :PACKED_BREADTH], hidden_multiplier)
    incoming_spun = spinning(hidden_squeeze[:, PACKED_BREADTH:], lengths)
    fresh_hidden = incoming_hidden.astype(jnp.bfloat16)
    fresh_spun = incoming_spun.astype(jnp.bfloat16)
    asker_unspun = jnp.dot(squeezed, asker_unspun_matrix.reshape(ASK_PACKED, ASKER_COUNT * PLAIN_SPAN), preferred_element_type=jnp.float32)
    asker_unspun = asker_unspun.reshape(BATCH_COUNT, ASKER_COUNT, PLAIN_SPAN).astype(jnp.bfloat16)
    query_latent = jnp.einsum('bhd,hdc->bhc', asker_unspun.astype(jnp.float32), lock_widen_matrix.astype(jnp.float32)).astype(jnp.bfloat16)
    asker_spun = jnp.dot(squeezed, asker_spin_matrix.reshape(ASK_PACKED, ASKER_COUNT * SPIN_SPAN), preferred_element_type=jnp.float32)
    asker_spun = spinning(asker_spun.reshape(BATCH_COUNT, ASKER_COUNT, SPIN_SPAN), lengths).astype(jnp.bfloat16)
    positions = jnp.arange(MEMORY_SLOTS, dtype=jnp.int32)
    score_scale = (PLAIN_SPAN + SPIN_SPAN) ** (-0.5)

    def attend(per_sequence):
        one_latent, one_turned, keys_latent, keys_turned, fresh_latent, fresh_turned, length = per_sequence
        fresh_slot = positions == length
        keys_latent = jnp.where(fresh_slot[:, None], fresh_latent[None, :], keys_latent).astype(jnp.float32)
        keys_turned = jnp.where(fresh_slot[:, None], fresh_turned[None, :], keys_turned).astype(jnp.float32)
        scores = jnp.dot(one_latent.astype(jnp.float32), keys_latent.T) + jnp.dot(one_turned.astype(jnp.float32), keys_turned.T)
        scores = scores * score_scale
        visible = (positions <= length)[None, :]
        scores = jnp.where(visible, scores, -1e+30)
        highest = lax.optimization_barrier(jnp.max(scores, axis=1, keepdims=True))
        weights = jnp.where(visible, jnp.exp(scores - highest), 0.0)
        denominator = lax.optimization_barrier(jnp.sum(weights, axis=1, keepdims=True))
        rounded = lax.optimization_barrier(weights.astype(jnp.bfloat16)).astype(jnp.float32)
        mixture = jnp.dot(rounded, keys_latent)
        return (mixture / denominator).astype(jnp.bfloat16)
    attended = lax.map(attend, (query_latent, asker_spun, cache_latent, cache_rotary, fresh_hidden, fresh_spun, lengths))
    head_values = jnp.einsum('bhc,hcv->bhv', attended.astype(jnp.float32), payload_widen_matrix.astype(jnp.float32)).astype(jnp.bfloat16)
    output = jnp.dot(head_values.reshape(BATCH_COUNT, ASKER_COUNT * PAYLOAD_SPAN), w_output, preferred_element_type=jnp.float32)
    return (output, incoming_hidden, incoming_spun)
```

```python
import functools

import jax
import jax.numpy as jnp
from jax import lax
from jax.experimental import pallas as pl
from jax.experimental.pallas import tpu as pltpu
from jax.sharding import PartitionSpec as P

EPS = 1e-06
THETA = 10000.0
MESH = pl.DeviceIdType.MESH
F32 = jnp.float32
BF16 = jnp.bfloat16
NT = (((1,), (1,)), ((), ()))
CHUNKS = 4


def mm(a, b):
    return jnp.dot(a, b, preferred_element_type=F32)


def mm_nt(a, b):
    return lax.dot_general(a, b, NT, preferred_element_type=F32)


def swap_halves(x, half):
    width = x.shape[1]
    if width == 2 * half:
        return jnp.concatenate([x[:, half:], x[:, :half]], axis=1)
    lane = lax.broadcasted_iota(jnp.int32, x.shape, 1)
    ahead = pltpu.roll(x, width - half, 1)
    behind = pltpu.roll(x, half, 1)
    return jnp.where((lane & (2 * half - 1)) < half, ahead, behind)


def kernel(
    dims,
    tok, gain, qmul, hmul, cos_t, sin_t, len_t,
    narrow_h, hid_h, unspun_h, spin_h, lock_h, pay_h, wout_h, lat_h, rot_h,
    out_ref, hidden_ref, spun_ref,
    narrow_q, hid_l, hid_r, unspun, spin, lock, pay, wout, lat, rot,
    ra, sa, qs, qg, mo, mr, so, sr, at, po, pr,
    load_sem,
    a_send, a_recv, t_send, t_recv, q_send, q_recv, m_send, m_recv, s_send, s_recv, o_send, o_recv,
):
    n, nt, total_width, nope_w, rope_w = dims
    me = lax.axis_index("kv")
    mt = lax.axis_index("tp")
    seqs = tok.shape[0]
    heads = lock.shape[0]
    lat_w = lock.shape[2]
    q_w = qmul.shape[1]
    qh = narrow_q.shape[1]
    lh = hid_l.shape[0]
    span = lat.shape[1]
    half = rope_w // 2
    per = seqs // CHUNKS

    loads = []

    def load(src, dst):
        copy = pltpu.make_async_copy(src, dst, load_sem.at[len(loads)])
        copy.start()
        loads.append(copy)
        return copy

    l_narrow = load(narrow_h.at[:, pl.ds(pl.multiple_of(mt * qh, 128), qh)], narrow_q)
    l_hid = load(hid_h.at[pl.ds(pl.multiple_of(mt * lh, 128), lh), :], hid_l)
    l_hr = load(hid_h.at[pl.ds(lat_w, rope_w), :], hid_r)
    l_unspun = load(unspun_h, unspun)
    l_spin = load(spin_h, spin)
    l_lock = load(lock_h, lock)
    l_lat = load(lat_h, lat)
    l_rot = load(rot_h, rot)
    l_pay = load(pay_h, pay)
    l_wout = load(wout_h, wout)

    def peer(offset):
        return lax.rem(me + offset, n)

    barrier = pltpu.get_barrier_semaphore()
    for o in range(n):
        for t in range(nt):
            if o or t:
                pl.semaphore_signal(
                    barrier, inc=1, device_id={"kv": peer(o), "tp": lax.rem(mt + t, nt)}, device_id_type=MESH
                )

    def remote(src, dst, send, recv, where):
        return pltpu.make_async_remote_copy(
            src_ref=src, dst_ref=dst, send_sem=send, recv_sem=recv, device_id=where, device_id_type=MESH
        )

    started = []

    wide = tok[...].astype(F32)
    squares = jnp.sum(wide * wide, axis=1, keepdims=True)
    scaled = (wide * gain[...]).astype(BF16)
    l_narrow.wait()
    ra[me, :, :qh] = mm(scaled, narrow_q[...])
    l_hid.wait()
    ra[me, :, qh : qh + lh] = mm_nt(scaled, hid_l[...])
    l_hr.wait()
    ra[me, :, qh + lh : qh + lh + rope_w] = mm_nt(scaled, hid_r[...])
    ra[me, :, qh + lh + rope_w :] = jnp.broadcast_to(squares, (seqs, ra.shape[2] - qh - lh - rope_w))
    pl.semaphore_wait(barrier, n * nt - 1)
    for o in range(n - 1, 0, -1):
        copy = remote(ra.at[me], ra.at[me], a_send.at[o], a_recv.at[o], {"kv": peer(o)})
        copy.start()
        started.append(copy)
    for o in range(1, n):
        src = peer(n - o)
        remote(ra.at[me], ra.at[src], a_send.at[o], a_recv.at[o], {"kv": peer(o)}).wait_recv()
    total = ra[0]
    for j in range(1, n):
        total = total + ra[j]
    sa[mt] = total[:, : qh + lh]
    for t in range(1, nt):
        for i, (lo, size) in enumerate(((0, qh), (qh, lh))):
            part = sa.at[mt, :, pl.ds(lo, size)]
            copy = remote(part, part, t_send.at[t, i], t_recv.at[t, i], {"tp": lax.rem(mt + t, nt)})
            copy.start()
            started.append(copy)
    tail = total[:, qh + lh :]
    row_scale = lax.rsqrt(tail[:, rope_w : rope_w + 1] / total_width + EPS)

    def tp_wait(i, lo, size):
        for t in range(1, nt):
            src = lax.rem(mt + nt - t, nt)
            part = sa.at[src, :, pl.ds(lo, size)]
            remote(part, part, t_send.at[t, i], t_recv.at[t, i], {"tp": lax.rem(mt + t, nt)}).wait_recv()

    tp_wait(0, 0, qh)
    query_down = jnp.concatenate([sa[t, :, :qh] for t in range(nt)], axis=1) * row_scale
    mean_square = jnp.mean(query_down * query_down, axis=1, keepdims=True)
    squeezed = (query_down * lax.rsqrt(mean_square + EPS) * qmul[...]).astype(BF16)
    squeezed_wide = squeezed.astype(F32)

    tiles = q_w // 128
    stacked = jnp.concatenate([squeezed_wide[:, j * 128 : (j + 1) * 128] for j in range(tiles)], axis=0)
    row = lax.broadcasted_iota(jnp.int32, (128, 128 * heads), 0)
    col = lax.broadcasted_iota(jnp.int32, (128, 128 * heads), 1)
    first = row * heads
    repeat = jnp.where((col >= first) & (col < first + heads), 1.0, 0.0).astype(BF16)
    spread = mm(stacked.astype(BF16), repeat)
    head_of = lax.broadcasted_iota(jnp.int32, (seqs, 128 * heads), 1) & (heads - 1)
    l_unspun.wait()
    nope = None
    for j in range(tiles):
        piece = spread[j * seqs : (j + 1) * seqs]
        left = jnp.concatenate([jnp.where(head_of == h, piece, 0.0) for h in range(heads)], axis=0)
        term = mm(left.astype(BF16), unspun[j * 128 * heads : (j + 1) * 128 * heads, :])
        nope = term if nope is None else nope + term
    l_spin.wait()
    turned = mm_nt(squeezed, spin[...])
    turned = turned * cos_t[...] + swap_halves(turned, half) * sin_t[...]
    qs[:, :, lat_w:] = jnp.zeros((seqs, heads, qs.shape[2] - lat_w), F32)
    l_lock.wait()
    for h in range(heads):
        qs[:, h, lat_w : lat_w + rope_w] = turned[:, h * rope_w : (h + 1) * rope_w]
        qs[:, h, :lat_w] = mm(nope[h * seqs : (h + 1) * seqs].astype(BF16), lock[h])
    for c in range(CHUNKS):
        for b in range(c * per, (c + 1) * per):
            qg[me, b] = qs[b].astype(BF16)
        for o in range(n - 1, 0, -1):
            part = qg.at[me, pl.ds(c * per, per)]
            copy = remote(part, part, q_send.at[o, c], q_recv.at[o, c], {"kv": peer(o)})
            copy.start()
            started.append(copy)

    tp_wait(1, qh, lh)
    hid = jnp.concatenate([sa[t, :, qh:] for t in range(nt)], axis=1) * row_scale
    hid_square = jnp.mean(hid * hid, axis=1, keepdims=True)
    incoming = hid * lax.rsqrt(hid_square + EPS) * hmul[...]
    hidden_ref[...] = incoming
    fresh = incoming.astype(BF16).astype(F32)
    tail = tail * row_scale
    spun = tail[:, :rope_w] * cos_t[:, :rope_w] + swap_halves(tail, half)[:, :rope_w] * sin_t[:, :rope_w]
    spun_ref[...] = spun
    fresh_spun = spun.astype(BF16).astype(F32)

    all_heads = n * heads
    position = me * span + lax.broadcasted_iota(jnp.int32, (1, span), 1)
    lane = lax.broadcasted_iota(jnp.int32, (all_heads, 128), 1)
    stats = jnp.zeros((all_heads, 128), F32)
    scale = (nope_w + rope_w) ** (-0.5)
    l_lat.wait()
    l_rot.wait()
    for c in range(CHUNKS):
        for o in range(1, n):
            part = qg.at[peer(n - o), pl.ds(c * per, per)]
            remote(part, part, q_send.at[o, c], q_recv.at[o, c], {"kv": peer(o)}).wait_recv()
        for b in range(c * per, (c + 1) * per):
            query = jnp.concatenate([qg[j, b].astype(F32) for j in range(n)], axis=0)
            q_lat = query[:, :lat_w]
            q_rot = query[:, lat_w : lat_w + rope_w]
            keys = lat[b]
            length = len_t[b : b + 1, :]
            is_fresh = position == length
            visible = position <= length
            scores = mm_nt(q_lat.astype(BF16), keys) + mm(q_rot.astype(BF16), rot[b])
            fresh_score = jnp.sum(q_lat * fresh[b : b + 1, :], axis=1, keepdims=True) + jnp.sum(
                q_rot * fresh_spun[b : b + 1, :], axis=1, keepdims=True
            )
            scores = jnp.where(is_fresh, fresh_score, scores) * scale
            scores = jnp.where(visible, scores, -1e30)
            top = jnp.max(scores, axis=1, keepdims=True)
            weights = jnp.where(visible, jnp.exp(scores - top), 0.0)
            mass = jnp.sum(weights, axis=1, keepdims=True)
            rounded = weights.astype(BF16).astype(F32)
            fresh_weight = jnp.sum(jnp.where(is_fresh, rounded, 0.0), axis=1, keepdims=True)
            rounded = jnp.where(is_fresh, 0.0, rounded).astype(BF16)
            mix = mm(rounded, keys) + fresh_weight * fresh[b : b + 1, :]
            stats = jnp.where(lane == b, top, stats)
            stats = jnp.where(lane == seqs + b, mass, stats)
            for j in range(n):
                mo[j, b] = mix[j * heads : (j + 1) * heads].astype(BF16)
        for o in range(n - 1, 0, -1):
            to = peer(o)
            rows = pl.ds(c * per, per)
            copy = remote(mo.at[to, rows], mr.at[me, rows], m_send.at[o, c], m_recv.at[o, c], {"kv": to})
            copy.start()
            started.append(copy)
        if c == CHUNKS - 1:
            for j in range(n):
                so[j] = stats[j * heads : (j + 1) * heads]
            for o in range(n - 1, 0, -1):
                to = peer(o)
                copy = remote(so.at[to], sr.at[me], s_send.at[o], s_recv.at[o], {"kv": to})
                copy.start()
                started.append(copy)
    sr[me] = so[me]
    for b in range(seqs):
        mr[me, b] = mo[me, b]
    for o in range(1, n):
        src = peer(n - o)
        remote(so.at[src], sr.at[src], s_send.at[o], s_recv.at[o], {"kv": peer(o)}).wait_recv()
    all_stats = [sr[j] for j in range(n)]
    highest = all_stats[0]
    for s in all_stats[1:]:
        highest = jnp.maximum(highest, s)
    factors = [jnp.exp(jnp.minimum(s - highest, 0.0)) for s in all_stats]
    for c in range(CHUNKS):
        for o in range(1, n):
            src = peer(n - o)
            rows = pl.ds(c * per, per)
            remote(mo.at[src, rows], mr.at[src, rows], m_send.at[o, c], m_recv.at[o, c], {"kv": peer(o)}).wait_recv()
        for b in range(c * per, (c + 1) * per):
            mixture = None
            for j in range(n):
                f = factors[j][:, b : b + 1]
                term = mr[j, b].astype(F32) * f
                mass = all_stats[j][:, seqs + b : seqs + b + 1] * f
                mixture = term if mixture is None else mixture + term
                denominator = mass if j == 0 else denominator + mass
            at[b] = mixture / denominator

    l_pay.wait()
    values = jnp.concatenate([mm(at[:, h, :].astype(BF16), pay[h]) for h in range(heads)], axis=1).astype(BF16)
    l_wout.wait()
    block = out_ref.shape[1]
    mine = me * nt + mt
    for k in range(n * nt):
        po[k] = mm(values, wout[:, k * block : (k + 1) * block]).astype(BF16)

        @pl.when(mine != k)
        def _():
            remote(
                po.at[k], pr.at[mine], o_send.at[k], o_recv.at[mine], {"kv": k // nt, "tp": k % nt}
            ).start()

    pr[mine] = po[mine]
    for k in range(n * nt):

        @pl.when(mine != k)
        def _():
            remote(
                po.at[k], pr.at[k], o_send.at[k], o_recv.at[k], {"kv": k // nt, "tp": k % nt}
            ).wait()

    summed = pr[0].astype(F32)
    for k in range(1, n * nt):
        summed = summed + pr[k].astype(F32)
    out_ref[...] = summed
    for copy in started:
        copy.wait_send()


def local(
    n, nt,
    tokens, token_gain, asker_narrow_matrix, hidden_narrow_matrix, asker_multiplier, hidden_multiplier,
    asker_unspun_matrix, asker_spin_matrix, lock_widen_matrix, payload_widen_matrix, w_output,
    cache_latent, cache_rotary, lengths,
):
    seqs, width = tokens.shape
    q_w, heads, nope_w = asker_unspun_matrix.shape
    rope_w = asker_spin_matrix.shape[2]
    lat_w = lock_widen_matrix.shape[2]
    span = cache_latent.shape[1]
    model = w_output.shape[1]
    block = model // (n * nt)
    exponent = jnp.arange(rope_w // 2, dtype=F32) * (2.0 / rope_w)
    frequency = THETA ** (-exponent)
    sign = jnp.tile(jnp.repeat(jnp.array([-1.0, 1.0], F32), rope_w // 2), heads)
    angles = lengths.astype(F32)[:, None] * jnp.tile(frequency, 2 * heads)[None, :]
    cos_t = jnp.cos(angles)
    sin_t = jnp.sin(angles) * sign[None, :]
    len_t = jnp.broadcast_to(lengths[:, None], (seqs, span))
    qh, lh = q_w // nt, lat_w // nt
    tail = max(128, 2 * rope_w)
    qs_w = lat_w + max(128, rope_w)
    vm = pl.BlockSpec(memory_space=pltpu.VMEM)
    hbm = pl.BlockSpec(memory_space=pl.ANY)
    dma = pltpu.SemaphoreType.DMA
    operands = (
        tokens, token_gain[None, :], asker_multiplier[None, :], hidden_multiplier[None, :], cos_t, sin_t, len_t,
        asker_narrow_matrix,
        hidden_narrow_matrix.T,
        asker_unspun_matrix.reshape(q_w * heads, nope_w),
        asker_spin_matrix.transpose(1, 2, 0).reshape(heads * rope_w, q_w),
        lock_widen_matrix, payload_widen_matrix, w_output, cache_latent,
        cache_rotary.transpose(0, 2, 1),
    )
    scratch = [
        pltpu.VMEM((width, qh), BF16),
        pltpu.VMEM((lh, width), BF16),
        pltpu.VMEM((rope_w, width), BF16),
        pltpu.VMEM((q_w * heads, nope_w), BF16),
        pltpu.VMEM((heads * rope_w, q_w), BF16),
        pltpu.VMEM(lock_widen_matrix.shape, BF16),
        pltpu.VMEM(payload_widen_matrix.shape, BF16),
        pltpu.VMEM(w_output.shape, BF16),
        pltpu.VMEM(cache_latent.shape, BF16),
        pltpu.VMEM((seqs, rope_w, span), BF16),
        pltpu.VMEM((n, seqs, qh + lh + tail), F32),
        pltpu.VMEM((nt, seqs, qh + lh), F32),
        pltpu.VMEM((seqs, heads, qs_w), F32),
        pltpu.VMEM((n, seqs, heads, qs_w), BF16),
        pltpu.VMEM((n, seqs, heads, lat_w), BF16),
        pltpu.VMEM((n, seqs, heads, lat_w), BF16),
        pltpu.VMEM((n, heads, 128), F32),
        pltpu.VMEM((n, heads, 128), F32),
        pltpu.VMEM((seqs, heads, lat_w), F32),
        pltpu.VMEM((n * nt, seqs, block), BF16),
        pltpu.VMEM((n * nt, seqs, block), BF16),
        dma((10,)),
        dma((n,)), dma((n,)),
        dma((nt, 2)), dma((nt, 2)),
        dma((n, CHUNKS)), dma((n, CHUNKS)),
        dma((n, CHUNKS)), dma((n, CHUNKS)),
        dma((n,)), dma((n,)),
        dma((n * nt,)), dma((n * nt,)),
    ]
    return pl.pallas_call(
        functools.partial(kernel, (n, nt, width * n, nope_w, rope_w)),
        out_shape=(
            jax.ShapeDtypeStruct((seqs, block), F32),
            jax.ShapeDtypeStruct((seqs, lat_w), F32),
            jax.ShapeDtypeStruct((seqs, rope_w), F32),
        ),
        in_specs=[vm] * 7 + [hbm] * 9,
        out_specs=(vm, vm, vm),
        scratch_shapes=scratch,
        compiler_params=pltpu.CompilerParams(
            collective_id=0, has_side_effects=True, vmem_limit_bytes=60 * 1024 * 1024
        ),
    )(*operands)


def solution(mesh):
    return jax.shard_map(
        functools.partial(local, mesh.shape["kv"], mesh.shape["tp"]),
        mesh=mesh,
        in_specs=(
            P("dp", "kv"),
            P("kv"),
            P("kv", None),
            P("kv", None),
            P(),
            P(),
            P(None, ("kv", "tp"), None),
            P(None, ("kv", "tp"), None),
            P(("kv", "tp"), None, None),
            P(("kv", "tp"), None, None),
            P(("kv", "tp"), None),
            P("dp", "kv", None),
            P("dp", "kv", None),
            P("dp"),
        ),
        out_specs=(P("dp", ("kv", "tp")), P("dp", None), P("dp", None)),
        check_vma=False,
    )
```

```python
import functools

import jax
import jax.numpy as jnp
import numpy as np
from jax import lax
from jax.experimental import pallas as pl
from jax.experimental.pallas import tpu as pltpu
from jax.sharding import PartitionSpec as P

EPS = 1e-06
THETA = 10000.0
MESH = pl.DeviceIdType.MESH
F32 = jnp.float32
BF16 = jnp.bfloat16
NT = (((1,), (1,)), ((), ()))
CHUNKS = 4


def mm(a, b):
    return jnp.dot(a, b, preferred_element_type=F32)


def mm_nt(a, b):
    return lax.dot_general(a, b, NT, preferred_element_type=F32)


def swap_halves(x, half):
    width = x.shape[1]
    if width == 2 * half:
        return jnp.concatenate([x[:, half:], x[:, :half]], axis=1)
    lane = lax.broadcasted_iota(jnp.int32, x.shape, 1)
    ahead = pltpu.roll(x, width - half, 1)
    behind = pltpu.roll(x, half, 1)
    return jnp.where((lane & (2 * half - 1)) < half, ahead, behind)


def kernel(
    dims,
    lens, tok, gain, qmul_t, hmul, freq,
    narrow_h, hid_h, unspun_h, spin_h, lock_h, pay_h, wout_h, lat_h, rot_h,
    out_ref, hidden_ref, spun_ref,
    narrow_q, hid_l, hid_r, unspun, spin, lock, pay, wout, lat, rot,
    ra, rh, sa, qs, qg, mo, mr, so, sr, at, po, pr,
    load_sem,
    a_send, a_recv, h_send, h_recv, t_send, t_recv, q_send, q_recv, m_send, m_recv, s_send, s_recv, o_send, o_recv,
):
    n, nt, total_width, nope_w, rope_w = dims
    me = lax.axis_index("kv")
    mt = lax.axis_index("tp")
    seqs = tok.shape[0]
    heads = lock.shape[0]
    lat_w = lock.shape[2]
    q_w = qmul_t.shape[0] * qmul_t.shape[1]
    qh = narrow_q.shape[1]
    lh = hid_l.shape[0]
    span = lat.shape[1]
    half = rope_w // 2
    per = seqs // CHUNKS

    loads = []

    def load(src, dst):
        copy = pltpu.make_async_copy(src, dst, load_sem.at[len(loads)])
        copy.start()
        loads.append(copy)
        return copy

    l_narrow = load(narrow_h.at[:, pl.ds(pl.multiple_of(mt * qh, 128), qh)], narrow_q)
    l_hid = load(hid_h.at[pl.ds(pl.multiple_of(mt * lh, 128), lh), :], hid_l)
    l_hr = load(hid_h.at[pl.ds(lat_w, rope_w), :], hid_r)
    def peer(offset):
        return lax.rem(me + offset, n)

    barrier = pltpu.get_barrier_semaphore()
    for o in range(n):
        for t in range(nt):
            if o or t:
                pl.semaphore_signal(
                    barrier, inc=1, device_id={"kv": peer(o), "tp": lax.rem(mt + t, nt)}, device_id_type=MESH
                )

    def remote(src, dst, send, recv, where):
        return pltpu.make_async_remote_copy(
            src_ref=src, dst_ref=dst, send_sem=send, recv_sem=recv, device_id=where, device_id_type=MESH
        )

    started = []

    seq_row = lax.broadcasted_iota(jnp.int32, (seqs, 1), 0)
    length_col = jnp.zeros((seqs, 1), jnp.int32)
    for b in range(seqs):
        length_col = jnp.where(seq_row == b, lens[b], length_col)
    angles = length_col.astype(F32) * freq[...]
    cos_t = jnp.cos(angles)
    sin_t = jnp.sin(angles)
    in_former = (lax.broadcasted_iota(jnp.int32, angles.shape, 1) & (rope_w - 1)) < half
    sin_t = jnp.where(in_former, -sin_t, sin_t)
    qmul = jnp.concatenate([qmul_t[j : j + 1, :] for j in range(qmul_t.shape[0])], axis=1)

    wide = tok[...].astype(F32)
    squares = jnp.sum(wide * wide, axis=1, keepdims=True)
    scaled = (wide * gain[...]).astype(BF16)
    l_narrow.wait()
    l_hr.wait()
    ra[me, :, :qh] = mm(scaled, narrow_q[...])
    ra[me, :, qh : qh + rope_w] = mm_nt(scaled, hid_r[...])
    ra[me, :, qh + rope_w :] = jnp.broadcast_to(squares, (seqs, ra.shape[2] - qh - rope_w))
    pl.semaphore_wait(barrier, n * nt - 1)
    for o in range(n - 1, 0, -1):
        copy = remote(ra.at[me], ra.at[me], a_send.at[o], a_recv.at[o], {"kv": peer(o)})
        copy.start()
        started.append(copy)
    l_hid.wait()
    l_unspun = load(unspun_h, unspun)
    l_spin = load(spin_h, spin)
    l_lock = load(lock_h, lock)
    rh[me] = mm_nt(scaled, hid_l[...])
    for o in range(n - 1, 0, -1):
        copy = remote(rh.at[me], rh.at[me], h_send.at[o], h_recv.at[o], {"kv": peer(o)})
        copy.start()
        started.append(copy)

    def tp_send(i, lo, size):
        part = sa.at[mt, :, pl.ds(lo, size)]
        for t in range(1, nt):
            copy = remote(part, part, t_send.at[t, i], t_recv.at[t, i], {"tp": lax.rem(mt + t, nt)})
            copy.start()
            started.append(copy)

    for o in range(1, n):
        src = peer(n - o)
        remote(ra.at[me], ra.at[src], a_send.at[o], a_recv.at[o], {"kv": peer(o)}).wait_recv()
    total = ra[0]
    for j in range(1, n):
        total = total + ra[j]
    sa[mt, :, :qh] = total[:, :qh]
    tp_send(0, 0, qh)
    l_lat = load(lat_h, lat)
    l_rot = load(rot_h, rot)
    l_pay = load(pay_h, pay)
    l_wout = load(wout_h, wout)
    tail = total[:, qh:]
    row_scale = lax.rsqrt(tail[:, rope_w : rope_w + 1] / total_width + EPS)

    def tp_wait(i, lo, size):
        for t in range(1, nt):
            src = lax.rem(mt + nt - t, nt)
            part = sa.at[src, :, pl.ds(lo, size)]
            remote(part, part, t_send.at[t, i], t_recv.at[t, i], {"tp": lax.rem(mt + t, nt)}).wait_recv()

    tp_wait(0, 0, qh)
    query_down = jnp.concatenate([sa[t, :, :qh] for t in range(nt)], axis=1) * row_scale
    mean_square = jnp.mean(query_down * query_down, axis=1, keepdims=True)
    squeezed = (query_down * lax.rsqrt(mean_square + EPS) * qmul).astype(BF16)
    squeezed_wide = squeezed.astype(F32)

    tiles = q_w // 128
    stacked = jnp.concatenate([squeezed_wide[:, j * 128 : (j + 1) * 128] for j in range(tiles)], axis=0)
    row = lax.broadcasted_iota(jnp.int32, (128, 128 * heads), 0)
    col = lax.broadcasted_iota(jnp.int32, (128, 128 * heads), 1)
    first = row * heads
    repeat = jnp.where((col >= first) & (col < first + heads), 1.0, 0.0).astype(BF16)
    spread = mm(stacked.astype(BF16), repeat)
    head_of = lax.broadcasted_iota(jnp.int32, (seqs, 128 * heads), 1) & (heads - 1)
    l_unspun.wait()
    nope = None
    for j in range(tiles):
        piece = spread[j * seqs : (j + 1) * seqs]
        left = jnp.concatenate([jnp.where(head_of == h, piece, 0.0) for h in range(heads)], axis=0)
        term = mm(left.astype(BF16), unspun[j * 128 * heads : (j + 1) * 128 * heads, :])
        nope = term if nope is None else nope + term
    l_spin.wait()
    turned = mm_nt(squeezed, spin[...])
    turned = turned * cos_t + swap_halves(turned, half) * sin_t
    qs[:, :, lat_w:] = jnp.zeros((seqs, heads, qs.shape[2] - lat_w), F32)
    l_lock.wait()
    for h in range(heads):
        qs[:, h, lat_w : lat_w + rope_w] = turned[:, h * rope_w : (h + 1) * rope_w]
        qs[:, h, :lat_w] = mm(nope[h * seqs : (h + 1) * seqs].astype(BF16), lock[h])
    for c in range(CHUNKS):
        for b in range(c * per, (c + 1) * per):
            qg[me, b] = qs[b].astype(BF16)
        for o in range(n - 1, 0, -1):
            part = qg.at[me, pl.ds(c * per, per)]
            copy = remote(part, part, q_send.at[o, c], q_recv.at[o, c], {"kv": peer(o)})
            copy.start()
            started.append(copy)

    for o in range(1, n):
        src = peer(n - o)
        remote(rh.at[me], rh.at[src], h_send.at[o], h_recv.at[o], {"kv": peer(o)}).wait_recv()
    total = rh[0]
    for j in range(1, n):
        total = total + rh[j]
    sa[mt, :, qh:] = total
    tp_send(1, qh, lh)
    tp_wait(1, qh, lh)
    hid = jnp.concatenate([sa[t, :, qh:] for t in range(nt)], axis=1) * row_scale
    hid_square = jnp.mean(hid * hid, axis=1, keepdims=True)
    incoming = hid * lax.rsqrt(hid_square + EPS) * hmul[...]
    hidden_ref[...] = incoming
    fresh = incoming.astype(BF16).astype(F32)
    tail = tail * row_scale
    spun = tail[:, :rope_w] * cos_t[:, :rope_w] + swap_halves(tail, half)[:, :rope_w] * sin_t[:, :rope_w]
    spun_ref[...] = spun
    fresh_spun = spun.astype(BF16).astype(F32)

    all_heads = n * heads
    position = me * span + lax.broadcasted_iota(jnp.int32, (1, span), 1)
    lane = lax.broadcasted_iota(jnp.int32, (all_heads, 128), 1)
    stats = jnp.zeros((all_heads, 128), F32)
    scale = (nope_w + rope_w) ** (-0.5)
    l_lat.wait()
    l_rot.wait()
    for c in range(CHUNKS):
        for o in range(1, n):
            part = qg.at[peer(n - o), pl.ds(c * per, per)]
            remote(part, part, q_send.at[o, c], q_recv.at[o, c], {"kv": peer(o)}).wait_recv()
        for b in range(c * per, (c + 1) * per):
            query = jnp.concatenate([qg[j, b].astype(F32) for j in range(n)], axis=0)
            q_lat = query[:, :lat_w]
            q_rot = query[:, lat_w : lat_w + rope_w]
            keys = lat[b]
            length = lens[b]
            is_fresh = position == length
            visible = position <= length
            scores = mm_nt(q_lat.astype(BF16), keys) + mm(q_rot.astype(BF16), rot[b])
            fresh_score = jnp.sum(q_lat * fresh[b : b + 1, :], axis=1, keepdims=True) + jnp.sum(
                q_rot * fresh_spun[b : b + 1, :], axis=1, keepdims=True
            )
            scores = jnp.where(is_fresh, fresh_score, scores) * scale
            scores = jnp.where(visible, scores, -1e30)
            top = jnp.max(scores, axis=1, keepdims=True)
            weights = jnp.where(visible, jnp.exp(scores - top), 0.0)
            mass = jnp.sum(weights, axis=1, keepdims=True)
            rounded = weights.astype(BF16).astype(F32)
            fresh_weight = jnp.sum(jnp.where(is_fresh, rounded, 0.0), axis=1, keepdims=True)
            rounded = jnp.where(is_fresh, 0.0, rounded).astype(BF16)
            mix = mm(rounded, keys) + fresh_weight * fresh[b : b + 1, :]
            stats = jnp.where(lane == b, top, stats)
            stats = jnp.where(lane == seqs + b, mass, stats)
            for j in range(n):
                mo[j, b] = mix[j * heads : (j + 1) * heads].astype(BF16)
        for o in range(n - 1, 0, -1):
            to = peer(o)
            rows = pl.ds(c * per, per)
            copy = remote(mo.at[to, rows], mr.at[me, rows], m_send.at[o, c], m_recv.at[o, c], {"kv": to})
            copy.start()
            started.append(copy)
        if c == CHUNKS - 1:
            for j in range(n):
                so[j] = stats[j * heads : (j + 1) * heads]
            for o in range(n - 1, 0, -1):
                to = peer(o)
                copy = remote(so.at[to], sr.at[me], s_send.at[o], s_recv.at[o], {"kv": to})
                copy.start()
                started.append(copy)
    sr[me] = so[me]
    for b in range(seqs):
        mr[me, b] = mo[me, b]
    for o in range(1, n):
        src = peer(n - o)
        remote(so.at[src], sr.at[src], s_send.at[o], s_recv.at[o], {"kv": peer(o)}).wait_recv()
    all_stats = [sr[j] for j in range(n)]
    highest = all_stats[0]
    for s in all_stats[1:]:
        highest = jnp.maximum(highest, s)
    factors = [jnp.exp(jnp.minimum(s - highest, 0.0)) for s in all_stats]
    for c in range(CHUNKS):
        for o in range(1, n):
            src = peer(n - o)
            rows = pl.ds(c * per, per)
            remote(mo.at[src, rows], mr.at[src, rows], m_send.at[o, c], m_recv.at[o, c], {"kv": peer(o)}).wait_recv()
        for b in range(c * per, (c + 1) * per):
            mixture = None
            for j in range(n):
                f = factors[j][:, b : b + 1]
                term = mr[j, b].astype(F32) * f
                mass = all_stats[j][:, seqs + b : seqs + b + 1] * f
                mixture = term if mixture is None else mixture + term
                denominator = mass if j == 0 else denominator + mass
            at[b] = mixture / denominator

    l_pay.wait()
    values = jnp.concatenate([mm(at[:, h, :].astype(BF16), pay[h]) for h in range(heads)], axis=1).astype(BF16)
    l_wout.wait()
    block = out_ref.shape[1]
    mine = me * nt + mt
    for k in range(n * nt):
        po[k] = mm(values, wout[:, k * block : (k + 1) * block]).astype(BF16)

        @pl.when(mine != k)
        def _():
            remote(
                po.at[k], pr.at[mine], o_send.at[k], o_recv.at[mine], {"kv": k // nt, "tp": k % nt}
            ).start()

    pr[mine] = po[mine]
    for k in range(n * nt):

        @pl.when(mine != k)
        def _():
            remote(
                po.at[k], pr.at[k], o_send.at[k], o_recv.at[k], {"kv": k // nt, "tp": k % nt}
            ).wait()

    summed = pr[0].astype(F32)
    for k in range(1, n * nt):
        summed = summed + pr[k].astype(F32)
    out_ref[...] = summed
    for copy in started:
        copy.wait_send()


def hand_on(*refs):
    for source, target in zip(refs[:3], refs[3:]):
        target[...] = source[...]


def local(
    n, nt,
    tokens, token_gain, asker_narrow_matrix, hidden_narrow_matrix, asker_multiplier, hidden_multiplier,
    asker_unspun_matrix, asker_spin_matrix, lock_widen_matrix, payload_widen_matrix, w_output,
    cache_latent, cache_rotary, lengths,
):
    seqs, width = tokens.shape
    q_w, heads, nope_w = asker_unspun_matrix.shape
    rope_w = asker_spin_matrix.shape[2]
    lat_w = lock_widen_matrix.shape[2]
    span = cache_latent.shape[1]
    model = w_output.shape[1]
    block = model // (n * nt)
    frequency = THETA ** (-np.arange(rope_w // 2) * (2.0 / rope_w))
    freq = np.tile(frequency, 2 * heads)[None, :].astype(np.float32)
    qh, lh = q_w // nt, lat_w // nt
    tail = max(128, 2 * rope_w)
    qs_w = lat_w + max(128, rope_w)
    vm = pl.BlockSpec(memory_space=pltpu.VMEM)
    hbm = pl.BlockSpec(memory_space=pl.ANY)
    dma = pltpu.SemaphoreType.DMA
    operands = (
        lengths, tokens, token_gain[None, :], asker_multiplier.reshape(-1, 128), hidden_multiplier[None, :], freq,
        asker_narrow_matrix,
        hidden_narrow_matrix.T,
        asker_unspun_matrix.reshape(q_w * heads, nope_w),
        asker_spin_matrix.transpose(1, 2, 0).reshape(heads * rope_w, q_w),
        lock_widen_matrix, payload_widen_matrix, w_output, cache_latent,
        cache_rotary.transpose(0, 2, 1),
    )
    scratch = [
        pltpu.VMEM((width, qh), BF16),
        pltpu.VMEM((lh, width), BF16),
        pltpu.VMEM((rope_w, width), BF16),
        pltpu.VMEM((q_w * heads, nope_w), BF16),
        pltpu.VMEM((heads * rope_w, q_w), BF16),
        pltpu.VMEM(lock_widen_matrix.shape, BF16),
        pltpu.VMEM(payload_widen_matrix.shape, BF16),
        pltpu.VMEM(w_output.shape, BF16),
        pltpu.VMEM(cache_latent.shape, BF16),
        pltpu.VMEM((seqs, rope_w, span), BF16),
        pltpu.VMEM((n, seqs, qh + tail), F32),
        pltpu.VMEM((n, seqs, lh), F32),
        pltpu.VMEM((nt, seqs, qh + lh), F32),
        pltpu.VMEM((seqs, heads, qs_w), F32),
        pltpu.VMEM((n, seqs, heads, qs_w), BF16),
        pltpu.VMEM((n, seqs, heads, lat_w), BF16),
        pltpu.VMEM((n, seqs, heads, lat_w), BF16),
        pltpu.VMEM((n, heads, 128), F32),
        pltpu.VMEM((n, heads, 128), F32),
        pltpu.VMEM((seqs, heads, lat_w), F32),
        pltpu.VMEM((n * nt, seqs, block), BF16),
        pltpu.VMEM((n * nt, seqs, block), BF16),
        dma((10,)),
        dma((n,)), dma((n,)),
        dma((n,)), dma((n,)),
        dma((nt, 2)), dma((nt, 2)),
        dma((n, CHUNKS)), dma((n, CHUNKS)),
        dma((n, CHUNKS)), dma((n, CHUNKS)),
        dma((n,)), dma((n,)),
        dma((n * nt,)), dma((n * nt,)),
    ]
    results = pl.pallas_call(
        functools.partial(kernel, (n, nt, width * n, nope_w, rope_w)),
        out_shape=(
            jax.ShapeDtypeStruct((seqs, block), F32),
            jax.ShapeDtypeStruct((seqs, lat_w), F32),
            jax.ShapeDtypeStruct((seqs, rope_w), F32),
        ),
        in_specs=[pl.BlockSpec(memory_space=pltpu.SMEM)] + [vm] * 5 + [hbm] * 9,
        out_specs=(vm, vm, vm),
        scratch_shapes=scratch,
        compiler_params=pltpu.CompilerParams(
            collective_id=0, has_side_effects=True, vmem_limit_bytes=60 * 1024 * 1024
        ),
    )(*operands)
    return pl.pallas_call(
        hand_on,
        out_shape=tuple(jax.ShapeDtypeStruct(x.shape, x.dtype) for x in results),
        in_specs=[vm] * 3,
        out_specs=(vm, vm, vm),
    )(*results)


def solution(mesh):
    return jax.shard_map(
        functools.partial(local, mesh.shape["kv"], mesh.shape["tp"]),
        mesh=mesh,
        in_specs=(
            P("dp", "kv"),
            P("kv"),
            P("kv", None),
            P("kv", None),
            P(),
            P(),
            P(None, ("kv", "tp"), None),
            P(None, ("kv", "tp"), None),
            P(("kv", "tp"), None, None),
            P(("kv", "tp"), None, None),
            P(("kv", "tp"), None),
            P("dp", "kv", None),
            P("dp", "kv", None),
            P("dp"),
        ),
        out_specs=(P("dp", ("kv", "tp")), P("dp", None), P("dp", None)),
        check_vma=False,
    )
```

```python
import functools

import jax
import jax.numpy as jnp
import numpy as np
from jax import lax
from jax.experimental import pallas as pl
from jax.experimental.pallas import tpu as pltpu
from jax.sharding import PartitionSpec as P

EPS = 1e-06
THETA = 10000.0
MESH = pl.DeviceIdType.MESH
F32 = jnp.float32
BF16 = jnp.bfloat16
NT = (((1,), (1,)), ((), ()))
CHUNKS = 4


def mm(a, b):
    return jnp.dot(a, b, preferred_element_type=F32)


def mm_nt(a, b):
    return lax.dot_general(a, b, NT, preferred_element_type=F32)


def swap_halves(x, half):
    width = x.shape[1]
    if width == 2 * half:
        return jnp.concatenate([x[:, half:], x[:, :half]], axis=1)
    lane = lax.broadcasted_iota(jnp.int32, x.shape, 1)
    ahead = pltpu.roll(x, width - half, 1)
    behind = pltpu.roll(x, half, 1)
    return jnp.where((lane & (2 * half - 1)) < half, ahead, behind)


def kernel(
    dims,
    lens, tok, gain, qmul_t, hmul, freq,
    narrow_h, hid_h, unspun_h, spin_h, lock_h, pay_h, wout_h, lat_h, rot_h,
    out_ref, hidden_ref, spun_ref,
    narrow_q, hid_l, hid_r, unspun, spin, lock, pay, wout, lat, rot,
    ra, rh, sa, qs, qg, mo, mr, so, sr, at, po, pr,
    load_sem,
    a_send, a_recv, h_send, h_recv, t_send, t_recv, q_send, q_recv, m_send, m_recv, s_send, s_recv, o_send, o_recv,
):
    n, nt, total_width, nope_w, rope_w = dims
    me = lax.axis_index("kv")
    mt = lax.axis_index("tp")
    seqs = tok.shape[0]
    heads = lock.shape[0]
    lat_w = lock.shape[2]
    q_w = qmul_t.shape[0] * qmul_t.shape[1]
    qh = narrow_q.shape[1]
    lh = hid_l.shape[0]
    span = lat.shape[1]
    half = rope_w // 2
    per = seqs // CHUNKS

    loads = []

    def load(src, dst):
        copy = pltpu.make_async_copy(src, dst, load_sem.at[len(loads)])
        copy.start()
        loads.append(copy)
        return copy

    l_narrow = load(narrow_h.at[:, pl.ds(pl.multiple_of(mt * qh, 128), qh)], narrow_q)
    l_hid = load(hid_h.at[pl.ds(pl.multiple_of(mt * lh, 128), lh), :], hid_l)
    l_hr = load(hid_h.at[pl.ds(lat_w, rope_w), :], hid_r)
    def peer(offset):
        return lax.rem(me + offset, n)

    barrier = pltpu.get_barrier_semaphore()
    for o in range(n):
        for t in range(nt):
            if o or t:
                pl.semaphore_signal(
                    barrier, inc=1, device_id={"kv": peer(o), "tp": lax.rem(mt + t, nt)}, device_id_type=MESH
                )

    def remote(src, dst, send, recv, where):
        return pltpu.make_async_remote_copy(
            src_ref=src, dst_ref=dst, send_sem=send, recv_sem=recv, device_id=where, device_id_type=MESH
        )

    started = []

    seq_row = lax.broadcasted_iota(jnp.int32, (seqs, 1), 0)
    length_col = jnp.zeros((seqs, 1), jnp.int32)
    for b in range(seqs):
        length_col = jnp.where(seq_row == b, lens[b], length_col)
    angles = length_col.astype(F32) * freq[...]
    cos_t = jnp.cos(angles)
    sin_t = jnp.sin(angles)
    in_former = (lax.broadcasted_iota(jnp.int32, angles.shape, 1) & (rope_w - 1)) < half
    sin_t = jnp.where(in_former, -sin_t, sin_t)
    qmul = jnp.concatenate([qmul_t[j : j + 1, :] for j in range(qmul_t.shape[0])], axis=1)

    wide = tok[...].astype(F32)
    squares = jnp.sum(wide * wide, axis=1, keepdims=True)
    scaled = (wide * gain[...]).astype(BF16)
    l_narrow.wait()
    l_hr.wait()
    ra[me, :, :qh] = mm(scaled, narrow_q[...])
    ra[me, :, qh : qh + rope_w] = mm_nt(scaled, hid_r[...])
    ra[me, :, qh + rope_w :] = jnp.broadcast_to(squares, (seqs, ra.shape[2] - qh - rope_w))
    pl.semaphore_wait(barrier, n * nt - 1)
    for o in range(n - 1, 0, -1):
        copy = remote(ra.at[me], ra.at[me], a_send.at[o], a_recv.at[o], {"kv": peer(o)})
        copy.start()
        started.append(copy)
    l_hid.wait()
    l_unspun = load(unspun_h, unspun)
    l_spin = load(spin_h, spin)
    l_lock = load(lock_h, lock)
    rh[me] = mm_nt(scaled, hid_l[...])
    for o in range(n - 1, 0, -1):
        copy = remote(rh.at[me], rh.at[me], h_send.at[o], h_recv.at[o], {"kv": peer(o)})
        copy.start()
        started.append(copy)

    def tp_send(i, lo, size):
        part = sa.at[mt, :, pl.ds(lo, size)]
        for t in range(1, nt):
            copy = remote(part, part, t_send.at[t, i], t_recv.at[t, i], {"tp": lax.rem(mt + t, nt)})
            copy.start()
            started.append(copy)

    for o in range(1, n):
        src = peer(n - o)
        remote(ra.at[me], ra.at[src], a_send.at[o], a_recv.at[o], {"kv": peer(o)}).wait_recv()
    total = ra[0]
    for j in range(1, n):
        total = total + ra[j]
    sa[mt, :, :qh] = total[:, :qh]
    tp_send(0, 0, qh)
    l_lat = load(lat_h, lat)
    l_rot = load(rot_h, rot)
    l_pay = load(pay_h, pay)
    l_wout = load(wout_h, wout)
    tail = total[:, qh:]
    row_scale = lax.rsqrt(tail[:, rope_w : rope_w + 1] / total_width + EPS)

    def tp_wait(i, lo, size):
        for t in range(1, nt):
            src = lax.rem(mt + nt - t, nt)
            part = sa.at[src, :, pl.ds(lo, size)]
            remote(part, part, t_send.at[t, i], t_recv.at[t, i], {"tp": lax.rem(mt + t, nt)}).wait_recv()

    tp_wait(0, 0, qh)
    query_down = jnp.concatenate([sa[t, :, :qh] for t in range(nt)], axis=1) * row_scale
    mean_square = jnp.mean(query_down * query_down, axis=1, keepdims=True)
    squeezed = (query_down * lax.rsqrt(mean_square + EPS) * qmul).astype(BF16)
    squeezed_wide = squeezed.astype(F32)

    bits = [1 << i for i in reversed(range(n.bit_length() - 1))]

    def across(offset):
        index = me
        for bit in bits:
            if offset & bit:
                index = index + bit - 2 * bit * lax.rem(index // bit, 2)
        return index

    def query_copy(held, bit, c):
        part = qg.at[across(held), pl.ds(c * per, per)]
        copy = remote(part, part, q_send.at[held ^ bit, c], q_recv.at[held ^ bit, c], {"kv": across(bit)})
        started.append(copy)
        return copy

    def query_wait(offset, bit, c):
        part = qg.at[across(offset), pl.ds(c * per, per)]
        remote(part, part, q_send.at[offset, c], q_recv.at[offset, c], {"kv": across(bit)}).wait_recv()

    def query_forward(c):
        held = [0]
        for bit in bits:
            for x in held[1:]:
                query_copy(x, bit, c).start()
            if bit > 1:
                for x in held:
                    query_wait(x ^ bit, bit, c)
                held = held + [x ^ bit for x in held]

    tiles = q_w // 128
    stacked = jnp.concatenate([squeezed_wide[:, j * 128 : (j + 1) * 128] for j in range(tiles)], axis=0)
    row = lax.broadcasted_iota(jnp.int32, (128, 128 * heads), 0)
    col = lax.broadcasted_iota(jnp.int32, (128, 128 * heads), 1)
    first = row * heads
    repeat = jnp.where((col >= first) & (col < first + heads), 1.0, 0.0).astype(BF16)
    spread = mm(stacked.astype(BF16), repeat)
    head_of = lax.broadcasted_iota(jnp.int32, (seqs, 128 * heads), 1) & (heads - 1)
    l_unspun.wait()
    nope = None
    for j in range(tiles):
        piece = spread[j * seqs : (j + 1) * seqs]
        left = jnp.concatenate([jnp.where(head_of == h, piece, 0.0) for h in range(heads)], axis=0)
        term = mm(left.astype(BF16), unspun[j * 128 * heads : (j + 1) * 128 * heads, :])
        nope = term if nope is None else nope + term
    l_spin.wait()
    turned = mm_nt(squeezed, spin[...])
    turned = turned * cos_t + swap_halves(turned, half) * sin_t
    qs[:, :, lat_w:] = jnp.zeros((seqs, heads, qs.shape[2] - lat_w), F32)
    l_lock.wait()
    for h in range(heads):
        qs[:, h, lat_w : lat_w + rope_w] = turned[:, h * rope_w : (h + 1) * rope_w]
        qs[:, h, :lat_w] = mm(nope[h * seqs : (h + 1) * seqs].astype(BF16), lock[h])
    for c in range(CHUNKS):
        for b in range(c * per, (c + 1) * per):
            qg[me, b] = qs[b].astype(BF16)
        for bit in bits:
            query_copy(0, bit, c).start()

    for o in range(1, n):
        src = peer(n - o)
        remote(rh.at[me], rh.at[src], h_send.at[o], h_recv.at[o], {"kv": peer(o)}).wait_recv()
    total = rh[0]
    for j in range(1, n):
        total = total + rh[j]
    sa[mt, :, qh:] = total
    tp_send(1, qh, lh)
    tp_wait(1, qh, lh)
    hid = jnp.concatenate([sa[t, :, qh:] for t in range(nt)], axis=1) * row_scale
    hid_square = jnp.mean(hid * hid, axis=1, keepdims=True)
    incoming = hid * lax.rsqrt(hid_square + EPS) * hmul[...]
    hidden_ref[...] = incoming
    fresh = incoming.astype(BF16).astype(F32)
    tail = tail * row_scale
    spun = tail[:, :rope_w] * cos_t[:, :rope_w] + swap_halves(tail, half)[:, :rope_w] * sin_t[:, :rope_w]
    spun_ref[...] = spun
    fresh_spun = spun.astype(BF16).astype(F32)

    all_heads = n * heads
    position = me * span + lax.broadcasted_iota(jnp.int32, (1, span), 1)
    lane = lax.broadcasted_iota(jnp.int32, (all_heads, 128), 1)
    stats = jnp.zeros((all_heads, 128), F32)
    scale = (nope_w + rope_w) ** (-0.5)
    l_lat.wait()
    l_rot.wait()
    for c in range(CHUNKS):
        if c == 0:
            query_forward(0)
        if c + 1 < CHUNKS:
            query_forward(c + 1)
        for offset in range(1, n, 2):
            query_wait(offset, 1, c)
        for b in range(c * per, (c + 1) * per):
            query = jnp.concatenate([qg[j, b].astype(F32) for j in range(n)], axis=0)
            q_lat = query[:, :lat_w]
            q_rot = query[:, lat_w : lat_w + rope_w]
            keys = lat[b]
            length = lens[b]
            is_fresh = position == length
            visible = position <= length
            scores = mm_nt(q_lat.astype(BF16), keys) + mm(q_rot.astype(BF16), rot[b])
            fresh_score = jnp.sum(q_lat * fresh[b : b + 1, :], axis=1, keepdims=True) + jnp.sum(
                q_rot * fresh_spun[b : b + 1, :], axis=1, keepdims=True
            )
            scores = jnp.where(is_fresh, fresh_score, scores) * scale
            scores = jnp.where(visible, scores, -1e30)
            top = jnp.max(scores, axis=1, keepdims=True)
            weights = jnp.where(visible, jnp.exp(scores - top), 0.0)
            mass = jnp.sum(weights, axis=1, keepdims=True)
            rounded = weights.astype(BF16).astype(F32)
            fresh_weight = jnp.sum(jnp.where(is_fresh, rounded, 0.0), axis=1, keepdims=True)
            rounded = jnp.where(is_fresh, 0.0, rounded).astype(BF16)
            mix = mm(rounded, keys) + fresh_weight * fresh[b : b + 1, :]
            stats = jnp.where(lane == b, top, stats)
            stats = jnp.where(lane == seqs + b, mass, stats)
            for j in range(n):
                mo[j, b] = mix[j * heads : (j + 1) * heads].astype(BF16)
        for o in range(n - 1, 0, -1):
            to = peer(o)
            rows = pl.ds(c * per, per)
            copy = remote(mo.at[to, rows], mr.at[me, rows], m_send.at[o, c], m_recv.at[o, c], {"kv": to})
            copy.start()
            started.append(copy)
        if c == CHUNKS - 1:
            for j in range(n):
                so[j] = stats[j * heads : (j + 1) * heads]
            for o in range(n - 1, 0, -1):
                to = peer(o)
                copy = remote(so.at[to], sr.at[me], s_send.at[o], s_recv.at[o], {"kv": to})
                copy.start()
                started.append(copy)
    sr[me] = so[me]
    for b in range(seqs):
        mr[me, b] = mo[me, b]
    for o in range(1, n):
        src = peer(n - o)
        remote(so.at[src], sr.at[src], s_send.at[o], s_recv.at[o], {"kv": peer(o)}).wait_recv()
    all_stats = [sr[j] for j in range(n)]
    highest = all_stats[0]
    for s in all_stats[1:]:
        highest = jnp.maximum(highest, s)
    factors = [jnp.exp(jnp.minimum(s - highest, 0.0)) for s in all_stats]
    for c in range(CHUNKS):
        for o in range(1, n):
            src = peer(n - o)
            rows = pl.ds(c * per, per)
            remote(mo.at[src, rows], mr.at[src, rows], m_send.at[o, c], m_recv.at[o, c], {"kv": peer(o)}).wait_recv()
        for b in range(c * per, (c + 1) * per):
            mixture = None
            for j in range(n):
                f = factors[j][:, b : b + 1]
                term = mr[j, b].astype(F32) * f
                mass = all_stats[j][:, seqs + b : seqs + b + 1] * f
                mixture = term if mixture is None else mixture + term
                denominator = mass if j == 0 else denominator + mass
            at[b] = mixture / denominator

    l_pay.wait()
    values = jnp.concatenate([mm(at[:, h, :].astype(BF16), pay[h]) for h in range(heads)], axis=1).astype(BF16)
    l_wout.wait()
    block = out_ref.shape[1]
    mine = me * nt + mt
    for k in range(n * nt):
        po[k] = mm(values, wout[:, k * block : (k + 1) * block]).astype(BF16)

        @pl.when(mine != k)
        def _():
            remote(
                po.at[k], pr.at[mine], o_send.at[k], o_recv.at[mine], {"kv": k // nt, "tp": k % nt}
            ).start()

    pr[mine] = po[mine]
    for k in range(n * nt):

        @pl.when(mine != k)
        def _():
            remote(
                po.at[k], pr.at[k], o_send.at[k], o_recv.at[k], {"kv": k // nt, "tp": k % nt}
            ).wait()

    summed = pr[0].astype(F32)
    for k in range(1, n * nt):
        summed = summed + pr[k].astype(F32)
    out_ref[...] = summed
    for copy in started:
        copy.wait_send()


def hand_on(*refs):
    for source, target in zip(refs[:3], refs[3:]):
        target[...] = source[...]


def local(
    n, nt,
    tokens, token_gain, asker_narrow_matrix, hidden_narrow_matrix, asker_multiplier, hidden_multiplier,
    asker_unspun_matrix, asker_spin_matrix, lock_widen_matrix, payload_widen_matrix, w_output,
    cache_latent, cache_rotary, lengths,
):
    seqs, width = tokens.shape
    q_w, heads, nope_w = asker_unspun_matrix.shape
    rope_w = asker_spin_matrix.shape[2]
    lat_w = lock_widen_matrix.shape[2]
    span = cache_latent.shape[1]
    model = w_output.shape[1]
    block = model // (n * nt)
    frequency = THETA ** (-np.arange(rope_w // 2) * (2.0 / rope_w))
    freq = np.tile(frequency, 2 * heads)[None, :].astype(np.float32)
    qh, lh = q_w // nt, lat_w // nt
    tail = max(128, 2 * rope_w)
    qs_w = lat_w + max(128, rope_w)
    vm = pl.BlockSpec(memory_space=pltpu.VMEM)
    hbm = pl.BlockSpec(memory_space=pl.ANY)
    dma = pltpu.SemaphoreType.DMA
    operands = (
        lengths, tokens, token_gain[None, :], asker_multiplier.reshape(-1, 128), hidden_multiplier[None, :], freq,
        asker_narrow_matrix,
        hidden_narrow_matrix.T,
        asker_unspun_matrix.reshape(q_w * heads, nope_w),
        asker_spin_matrix.transpose(1, 2, 0).reshape(heads * rope_w, q_w),
        lock_widen_matrix, payload_widen_matrix, w_output, cache_latent,
        cache_rotary.transpose(0, 2, 1),
    )
    scratch = [
        pltpu.VMEM((width, qh), BF16),
        pltpu.VMEM((lh, width), BF16),
        pltpu.VMEM((rope_w, width), BF16),
        pltpu.VMEM((q_w * heads, nope_w), BF16),
        pltpu.VMEM((heads * rope_w, q_w), BF16),
        pltpu.VMEM(lock_widen_matrix.shape, BF16),
        pltpu.VMEM(payload_widen_matrix.shape, BF16),
        pltpu.VMEM(w_output.shape, BF16),
        pltpu.VMEM(cache_latent.shape, BF16),
        pltpu.VMEM((seqs, rope_w, span), BF16),
        pltpu.VMEM((n, seqs, qh + tail), F32),
        pltpu.VMEM((n, seqs, lh), F32),
        pltpu.VMEM((nt, seqs, qh + lh), F32),
        pltpu.VMEM((seqs, heads, qs_w), F32),
        pltpu.VMEM((n, seqs, heads, qs_w), BF16),
        pltpu.VMEM((n, seqs, heads, lat_w), BF16),
        pltpu.VMEM((n, seqs, heads, lat_w), BF16),
        pltpu.VMEM((n, heads, 128), F32),
        pltpu.VMEM((n, heads, 128), F32),
        pltpu.VMEM((seqs, heads, lat_w), F32),
        pltpu.VMEM((n * nt, seqs, block), BF16),
        pltpu.VMEM((n * nt, seqs, block), BF16),
        dma((10,)),
        dma((n,)), dma((n,)),
        dma((n,)), dma((n,)),
        dma((nt, 2)), dma((nt, 2)),
        dma((n, CHUNKS)), dma((n, CHUNKS)),
        dma((n, CHUNKS)), dma((n, CHUNKS)),
        dma((n,)), dma((n,)),
        dma((n * nt,)), dma((n * nt,)),
    ]
    results = pl.pallas_call(
        functools.partial(kernel, (n, nt, width * n, nope_w, rope_w)),
        out_shape=(
            jax.ShapeDtypeStruct((seqs, block), F32),
            jax.ShapeDtypeStruct((seqs, lat_w), F32),
            jax.ShapeDtypeStruct((seqs, rope_w), F32),
        ),
        in_specs=[pl.BlockSpec(memory_space=pltpu.SMEM)] + [vm] * 5 + [hbm] * 9,
        out_specs=(vm, vm, vm),
        scratch_shapes=scratch,
        compiler_params=pltpu.CompilerParams(
            collective_id=0, has_side_effects=True, vmem_limit_bytes=60 * 1024 * 1024
        ),
    )(*operands)
    return pl.pallas_call(
        hand_on,
        out_shape=tuple(jax.ShapeDtypeStruct(x.shape, x.dtype) for x in results),
        in_specs=[vm] * 3,
        out_specs=(vm, vm, vm),
    )(*results)


def solution(mesh):
    return jax.shard_map(
        functools.partial(local, mesh.shape["kv"], mesh.shape["tp"]),
        mesh=mesh,
        in_specs=(
            P("dp", "kv"),
            P("kv"),
            P("kv", None),
            P("kv", None),
            P(),
            P(),
            P(None, ("kv", "tp"), None),
            P(None, ("kv", "tp"), None),
            P(("kv", "tp"), None, None),
            P(("kv", "tp"), None, None),
            P(("kv", "tp"), None),
            P("dp", "kv", None),
            P("dp", "kv", None),
            P("dp"),
        ),
        out_specs=(P("dp", ("kv", "tp")), P("dp", None), P("dp", None)),
        check_vma=False,
    )
```
